32 devices in a mesh: dp: 4 (over y, x), kv: 4 (over z), tp: 2 (over core).
Axes of the slice: x: 2, y: 2, z: 4, core: 2. Of those that a mesh axis runs over, the one named last changes fastest.
Arguments:
- tokens: bfloat16 [1024, 4096], P('dp', ('kv', 'tp')), may hold values from -53 to 53
- carried_state: float32 [1024, 16, 128, 128], P(('dp', 'kv', 'tp')), may hold values from -9 to 9
- first_gain: float32 [4096], replicated, may hold values from 0.1 to 1.9
- first_gate: bfloat16 [4096, 11264], P(None, ('kv', 'tp')), may hold values from -0.09375 to 0.09375
- first_up: bfloat16 [4096, 11264], P(None, ('kv', 'tp')), may hold values from -0.09375 to 0.09375
- first_down: bfloat16 [11264, 4096], P(('kv', 'tp')), may hold values from -0.078125 to 0.078125
- mix_gain: float32 [4096], replicated, may hold values from 0.1 to 1.9
- query_weight: bfloat16 [4096, 2048], P(('kv', 'tp')), may hold values from -0.09375 to 0.09375
- forget_weight: bfloat16 [4096, 2048], P(('kv', 'tp')), may hold values from -0.09375 to 0.09375
- input_weight: bfloat16 [4096, 2048], P(('kv', 'tp')), may hold values from -0.09375 to 0.09375
- outgate_weight: bfloat16 [4096, 2048], P(('kv', 'tp')), may hold values from -0.09375 to 0.09375
- forget_floor: float32 [2048], replicated, may hold values from 0.05 to 0.9
- head_gain: float32 [128], replicated, may hold values from 0.1 to 1.9
- output_weight: bfloat16 [2048, 4096], P(None, ('kv', 'tp')), may hold values from -0.125 to 0.125
- second_gain: float32 [4096], replicated, may hold values from 0.1 to 1.9
- second_gate: bfloat16 [4096, 11264], P(None, ('kv', 'tp')), may hold values from -0.09375 to 0.09375
- second_up: bfloat16 [4096, 11264], P(None, ('kv', 'tp')), may hold values from -0.09375 to 0.09375
- second_down: bfloat16 [11264, 4096], P(('kv', 'tp')), may hold values from -0.078125 to 0.078125
Outputs:
- layer_out: bfloat16 [1024, 4096], P('dp', ('kv', 'tp'))
- next_state: float32 [1024, 16, 128, 128], P(('dp', 'kv', 'tp'))
The draws below stay inside these ranges and needn't reach their ends.
All inputs are finite; a program needn't handle non-finite values.
Results may differ from the reference program's by a relative error of at most 0.018.
Values may be sent and summed in bfloat16 or wider, within the bound.
A program may use at most 256 MiB of HBM per device.

```python
import jax
import jax.numpy as jnp
from jax import lax

D = 4096
FF = 11264
HEADS = 16
KEY = 128
VAL = 128
SEQS = 1024
KW = 2048
VW = 2048


def draw_tokens(key, part):
    keys = jax.random.split(jax.random.fold_in(key, 11), 3)
    row_scale = jnp.exp(jax.random.uniform(keys[0], (SEQS, 1), jnp.float32, jnp.log(0.3), jnp.log(3.0)))
    col_trend = jnp.exp(jnp.linspace(jnp.log(0.4), jnp.log(2.5), D)).astype(jnp.float32).reshape(1, D)
    rough = jax.random.uniform(keys[1], (1, D), jnp.float32, 0.6, 1.4)
    base = jnp.clip(jax.random.normal(keys[2], (SEQS, D), jnp.float32), -5.0, 5.0)
    return (base * rough * col_trend * row_scale).astype(jnp.bfloat16)


def strengthened(result, rng, source, target, shards_of, factor):
    owner, partner = [(jnp.arange(result.shape[axis_at]) // (result.shape[axis_at] // shards_of)).reshape([-1 if axis == axis_at else 1 for axis in range(result.ndim)]) for axis_at in (source, target)]
    chosen = jax.random.permutation(rng, shards_of)[partner]
    strong = (owner == chosen) | (owner == (partner + shards_of // 2) % shards_of)
    return jnp.where(strong, factor * result, result)


def block_scale(stream_key, shape, cuts, least, top_value):
    loudness = 1.0
    for dim, parts in cuts:
        heights = jax.random.uniform(jax.random.fold_in(jax.random.fold_in(stream_key, 6), dim), (parts,), jnp.float32, least / len(cuts), top_value / len(cuts))
        loudness = loudness * jnp.repeat(jnp.exp(heights), shape[dim] // parts).reshape((-1,) + (1,) * (len(shape) - 1 - dim))
    return loudness


def scatter_about(rng, shape, width, limit, cuts=(), dtype=jnp.bfloat16):
    values = width * jax.random.normal(rng, shape, jnp.float32)
    if cuts:
        values = values * block_scale(rng, shape, cuts, -0.22, 0.18)
    return jnp.clip(values, -limit, limit).astype(dtype)


def noise_with(rng, extent, spread, most, cuts, heavy, kind=jnp.bfloat16):
    values = spread * jax.random.normal(rng, extent, jnp.float32)
    if cuts:
        values = values * block_scale(rng, extent, cuts, -0.22, 0.18)
    return jnp.clip(strengthened(values, jax.random.fold_in(rng, 3), *heavy), -most, most).astype(kind)


def setup_inputs(seed: int = 0) -> dict:
    arg_keys = jax.random.split(jax.random.key(seed), 19)
    tokens = draw_tokens(jax.random.fold_in(arg_keys[18], 71), 0)
    carried_state = scatter_about(arg_keys[1], (SEQS, HEADS, KEY, VAL), 1.5, 9.0, ((0, 32),), jnp.float32)
    first_gain = jnp.clip(1.0 + 0.18 * jax.random.normal(arg_keys[2], (D,), jnp.float32), 0.1, 1.9)
    first_gate = scatter_about(arg_keys[3], (D, FF), D ** -0.5, 0.09375, ((1, 8),))
    first_up = scatter_about(arg_keys[4], (D, FF), D ** -0.5, 0.09375, ((1, 8),))
    first_down = noise_with(arg_keys[5], (FF, D), FF ** -0.5, 0.078125, ((0, 8),), (0, 1, 8, 2.0))
    mix_gain = jnp.clip(1.0 + 0.18 * jax.random.normal(arg_keys[6], (D,), jnp.float32), 0.1, 1.9)
    query_weight = scatter_about(arg_keys[7], (D, KW), D ** -0.5, 0.09375, ((0, 8),))
    forget_weight = scatter_about(arg_keys[8], (D, KW), D ** -0.5, 0.09375, ((0, 8),))
    input_weight = scatter_about(arg_keys[9], (D, VW), D ** -0.5, 0.09375, ((0, 8),))
    outgate_weight = scatter_about(arg_keys[10], (D, VW), D ** -0.5, 0.09375, ((0, 8),))
    forget_floor = jnp.clip(jax.random.uniform(arg_keys[11], (KW,), jnp.float32, 0.05, 0.9), 0.05, 0.9)
    head_gain = jnp.clip(1.0 + 0.18 * jax.random.normal(arg_keys[12], (VAL,), jnp.float32), 0.1, 1.9)
    output_weight = scatter_about(arg_keys[13], (VW, D), VW ** -0.5, 0.125, ((1, 8),))
    second_gain = jnp.clip(1.0 + 0.18 * jax.random.normal(arg_keys[14], (D,), jnp.float32), 0.1, 1.9)
    second_gate = scatter_about(arg_keys[15], (D, FF), D ** -0.5, 0.09375, ((1, 8),))
    second_up = scatter_about(arg_keys[16], (D, FF), D ** -0.5, 0.09375, ((1, 8),))
    second_down = noise_with(arg_keys[17], (FF, D), FF ** -0.5, 0.078125, ((0, 8),), (0, 1, 8, 2.0))
    return {"tokens": tokens, "carried_state": carried_state, "first_gain": first_gain, "first_gate": first_gate, "first_up": first_up, "first_down": first_down, "mix_gain": mix_gain, "query_weight": query_weight, "forget_weight": forget_weight, "input_weight": input_weight, "outgate_weight": outgate_weight, "forget_floor": forget_floor, "head_gain": head_gain, "output_weight": output_weight, "second_gain": second_gain, "second_gate": second_gate, "second_up": second_up, "second_down": second_down}


epsilon = 1e-06

def inverse_rms(entries):
    return lax.rsqrt(lax.optimization_barrier(jnp.mean(entries * entries, axis=-1, keepdims=True)) + epsilon)

def half_channel(inputs, gain_vec, gate_weight, up_weight, down_weight):
    widened = inputs.astype(jnp.float32)
    row_scale = inverse_rms(widened)
    scaled = (widened * gain_vec).astype(jnp.bfloat16)
    gate_acc = row_scale * jnp.dot(scaled, gate_weight, preferred_element_type=jnp.float32)
    up_acc = row_scale * jnp.dot(scaled, up_weight, preferred_element_type=jnp.float32)
    hidden = (jax.nn.silu(gate_acc) * up_acc).astype(jnp.bfloat16)
    return (widened + 0.5 * jnp.dot(hidden, down_weight, preferred_element_type=jnp.float32)).astype(jnp.bfloat16)

def reference(tokens, carried_state, first_gain, first_gate, first_up, first_down, mix_gain, query_weight, forget_weight, input_weight, outgate_weight, forget_floor, head_gain, output_weight, second_gain, second_gate, second_up, second_down):
    mixer_in = half_channel(tokens, first_gain, first_gate, first_up, first_down)
    widened = mixer_in.astype(jnp.float32)
    row_scale = inverse_rms(widened)
    scaled = (widened * mix_gain).astype(jnp.bfloat16)
    seq_count = tokens.shape[0]
    query_act = (row_scale * jnp.dot(scaled, query_weight, preferred_element_type=jnp.float32)).reshape(seq_count, HEADS, KEY)
    forget_pre = (row_scale * jnp.dot(scaled, forget_weight, preferred_element_type=jnp.float32)).reshape(seq_count, HEADS, KEY)
    input_val = (row_scale * jnp.dot(scaled, input_weight, preferred_element_type=jnp.float32)).reshape(seq_count, HEADS, VAL)
    gate_pre = (row_scale * jnp.dot(scaled, outgate_weight, preferred_element_type=jnp.float32)).reshape(seq_count, HEADS, VAL)
    floor_grid = forget_floor.reshape(HEADS, KEY)
    forget = floor_grid + (1.0 - floor_grid) * jax.nn.sigmoid(forget_pre)
    next_state = forget[..., None] * carried_state + (1.0 - forget)[..., None] * input_val[:, :, None, :]
    readout = lax.optimization_barrier(jnp.sum(next_state * jax.nn.silu(query_act)[..., None], axis=2))
    normed = readout * inverse_rms(readout) * head_gain
    mixer_out = (normed * jax.nn.silu(gate_pre)).reshape(seq_count, VW).astype(jnp.bfloat16)
    middle = (widened + jnp.dot(mixer_out, output_weight, preferred_element_type=jnp.float32)).astype(jnp.bfloat16)
    layer_out = half_channel(middle, second_gain, second_gate, second_up, second_down)
    return (layer_out, next_state)
```

```python
import functools

import jax
import jax.numpy as jnp
from jax import lax
from jax.experimental import pallas as pl
from jax.experimental.pallas import tpu as pltpu
from jax.sharding import PartitionSpec as P

epsilon = 1e-06
MESH = pl.DeviceIdType.MESH
VMEM_LIMIT = 62 * 1024 * 1024


def remote(src, dst, send_sem, recv_sem, kv, tp):
    return pltpu.make_async_remote_copy(
        src_ref=src,
        dst_ref=dst,
        send_sem=send_sem,
        recv_sem=recv_sem,
        device_id={"kv": kv, "tp": tp},
        device_id_type=MESH,
    )


def greet(me, core, chips):
    barrier = pltpu.get_barrier_semaphore()
    pl.semaphore_signal(
        barrier, inc=1, device_id={"kv": me, "tp": 1 - core}, device_id_type=MESH
    )
    for step in range(1, chips):
        pl.semaphore_signal(
            barrier,
            inc=1,
            device_id={"kv": lax.rem(me + step, chips), "tp": core},
            device_id_type=MESH,
        )
    pl.semaphore_wait(barrier, chips)


def gather_kernel(chips, own_ref, full_ref, local_sem, chip_send, sib_send, recv_sem):
    me = lax.axis_index("kv")
    core = lax.axis_index("tp")
    mine = me * 2 + core
    local = pltpu.make_async_copy(own_ref, full_ref.at[mine], local_sem)
    local.start()
    greet(me, core, chips)
    sends = []
    for step in range(1, chips):
        peer = lax.rem(me + chips - step, chips)
        copy = remote(
            own_ref, full_ref.at[mine], chip_send.at[step], recv_sem.at[mine], peer, core
        )
        copy.start()
        sends.append(copy)
    copy = remote(own_ref, full_ref.at[mine], sib_send.at[0], recv_sem.at[mine], me, 1 - core)
    copy.start()
    sends.append(copy)
    for step in range(1, chips):
        slot = lax.rem(me + step, chips) * 2 + core
        remote(
            full_ref.at[slot], full_ref.at[slot], chip_send.at[0], recv_sem.at[slot], me, 1 - core
        ).wait_recv()
        copy = remote(
            full_ref.at[slot], full_ref.at[slot], sib_send.at[step], recv_sem.at[slot], me, 1 - core
        )
        copy.start()
        sends.append(copy)
    for step in range(chips):
        slot = lax.rem(me + step, chips) * 2 + 1 - core
        remote(
            full_ref.at[slot], full_ref.at[slot], chip_send.at[0], recv_sem.at[slot], me, 1 - core
        ).wait_recv()
    for copy in sends:
        copy.wait_send()
    local.wait()


def gather_rows(own, chips, collective_id):
    blocks = chips * 2
    return pl.pallas_call(
        functools.partial(gather_kernel, chips),
        out_shape=jax.ShapeDtypeStruct((blocks,) + own.shape, own.dtype),
        in_specs=[pl.BlockSpec(memory_space=pltpu.VMEM)],
        out_specs=pl.BlockSpec(memory_space=pltpu.VMEM),
        scratch_shapes=[
            pltpu.SemaphoreType.DMA,
            pltpu.SemaphoreType.DMA((chips,)),
            pltpu.SemaphoreType.DMA((chips,)),
            pltpu.SemaphoreType.DMA((blocks,)),
        ],
        compiler_params=pltpu.CompilerParams(
            collective_id=collective_id, has_side_effects=True, vmem_limit_bytes=VMEM_LIMIT
        ),
    )(own)


def block_kernel(
    chips,
    own_ref,
    gain_ref,
    gate_hbm,
    up_hbm,
    down_hbm,
    out_ref,
    gate_w,
    up_w,
    down_w,
    cols,
    gate_acc,
    up_acc,
    squares,
    hidden,
    sib_out,
    sib_in,
    chip_out,
    chip_in,
    gate_sem,
    up_sem,
    down_sem,
    local_sem,
    chip_send,
    sib_send,
    recv_sem,
    sib_out_sem,
    sib_in_sem,
    chip_out_sem,
    chip_in_sem,
):
    me = lax.axis_index("kv")
    core = lax.axis_index("tp")
    mine = me * 2 + core
    rows, width = own_ref.shape
    full_width = width * chips * 2

    def gate_copy(j):
        at = pl.ds(pl.multiple_of(j * width, width), width)
        return pltpu.make_async_copy(gate_hbm.at[at, :], gate_w.at[j], gate_sem.at[j])

    def up_copy(j):
        at = pl.ds(pl.multiple_of(j * width, width), width)
        return pltpu.make_async_copy(up_hbm.at[at, :], up_w.at[j], up_sem.at[j])

    def down_copy(j):
        at = pl.ds(pl.multiple_of(j * width, width), width)
        return pltpu.make_async_copy(down_hbm.at[:, at], down_w.at[j], down_sem.at[j])

    local = pltpu.make_async_copy(own_ref, cols.at[mine], local_sem)
    local.start()

    @pl.loop(0, chips)
    def _(step):
        q = lax.rem(me + step, chips)
        for c in (core, 1 - core):
            gate_copy(q * 2 + c).start()
            up_copy(q * 2 + c).start()

    greet(me, core, chips)

    def share_copy(step):
        return remote(
            own_ref,
            cols.at[mine],
            chip_send.at[step],
            recv_sem.at[mine],
            lax.rem(me + chips - step, chips),
            core,
        )

    def pass_copy(slot, step):
        return remote(
            cols.at[slot], cols.at[slot], sib_send.at[step], recv_sem.at[slot], me, 1 - core
        )

    @pl.loop(1, chips)
    def _(step):
        share_copy(step).start()

    @pl.loop(0, chips)
    def _(step):
        q = lax.rem(me + 1 + step, chips)
        for c in (1 - core, core):
            down_copy(q * 2 + c).start()

    gate_acc[...] = jnp.zeros_like(gate_acc)
    up_acc[...] = jnp.zeros_like(up_acc)
    squares[...] = jnp.zeros_like(squares)
    local.wait()

    def take(j):
        block = cols[j].astype(jnp.float32)
        squares[...] += jnp.sum(block * block, axis=1, keepdims=True)
        scaled = (block * gain_ref[j]).astype(jnp.bfloat16)
        gate_copy(j).wait()
        gate_acc[...] += jnp.dot(scaled, gate_w[j], preferred_element_type=jnp.float32)
        up_copy(j).wait()
        up_acc[...] += jnp.dot(scaled, up_w[j], preferred_element_type=jnp.float32)

    @pl.loop(0, chips * 2)
    def _(turn):
        step = lax.div(turn, 2)
        other = lax.rem(turn, 2)
        q = lax.rem(me + step, chips)
        slot = q * 2 + lax.rem(core + other, 2)

        @pl.when(turn > 0)
        def _():
            pass_copy(slot, step).wait_recv()

        @pl.when(other == 0)
        def _():
            pass_copy(slot, step).start()

        take(slot)

    tile = 32

    @pl.loop(0, rows // tile)
    def _(i):
        at = pl.ds(pl.multiple_of(i * tile, tile), tile)
        row_scale = lax.rsqrt(squares[at, :] / full_width + epsilon)
        gate = row_scale * gate_acc[at, :]
        hidden[at, :] = (gate * jax.nn.sigmoid(gate) * (row_scale * up_acc[at, :])).astype(
            jnp.bfloat16
        )

    def branch(j):
        down_copy(j).wait()
        return 0.5 * jnp.dot(hidden[...], down_w[j], preferred_element_type=jnp.float32)

    def sib_copy(q):
        return remote(
            sib_out.at[q], sib_in.at[q], sib_out_sem.at[q], sib_in_sem.at[q], me, 1 - core
        )

    def chip_copy(q):
        return remote(
            chip_out.at[q], chip_in.at[me], chip_out_sem.at[q], chip_in_sem.at[me], q, core
        )

    @pl.loop(0, chips)
    def _(step):
        q = lax.rem(me + 1 + step, chips)
        sib_out[q] = branch(q * 2 + 1 - core).astype(jnp.bfloat16)
        sib_copy(q).start()
        part = branch(q * 2 + core)
        sib_copy(q).wait_recv()
        chip_out[q] = (part + sib_in[q].astype(jnp.float32)).astype(jnp.bfloat16)

        @pl.when(step < chips - 1)
        def _():
            chip_copy(q).start()

        @pl.when(step == chips - 1)
        def _():
            gate_acc[:, :width] = part + sib_in[q].astype(jnp.float32)

    total = gate_acc[:, :width] + own_ref[...].astype(jnp.float32)
    for step in range(1, chips):
        q = lax.rem(me + step, chips)
        remote(
            chip_out.at[q], chip_in.at[q], chip_out_sem.at[q], chip_in_sem.at[q], q, core
        ).wait_recv()
        total = total + chip_in[q].astype(jnp.float32)
    out_ref[...] = total.astype(out_ref.dtype)

    @pl.loop(0, chips)
    def _(step):
        slot = lax.rem(me + step, chips) * 2 + core
        pass_copy(slot, step).wait_send()
        sib_copy(step).wait_send()

    @pl.loop(1, chips)
    def _(step):
        share_copy(step).wait_send()
        chip_copy(lax.rem(me + step, chips)).wait_send()


def feed_forward(own, gain, gate, up, down, chips, collective_id):
    rows, width = own.shape
    units = gate.shape[1]
    blocks = chips * 2
    dma = pltpu.SemaphoreType.DMA
    acc_width = max(units, width)
    return pl.pallas_call(
        functools.partial(block_kernel, chips),
        out_shape=jax.ShapeDtypeStruct((rows, width), jnp.bfloat16),
        in_specs=[pl.BlockSpec(memory_space=pltpu.VMEM)] * 2
        + [pl.BlockSpec(memory_space=pl.ANY)] * 3,
        out_specs=pl.BlockSpec(memory_space=pltpu.VMEM),
        scratch_shapes=[
            pltpu.VMEM((blocks, width, units), jnp.bfloat16),
            pltpu.VMEM((blocks, width, units), jnp.bfloat16),
            pltpu.VMEM((blocks, units, width), jnp.bfloat16),
            pltpu.VMEM((blocks, rows, width), jnp.bfloat16),
            pltpu.VMEM((rows, units), jnp.float32),
            pltpu.VMEM((rows, units), jnp.float32),
            pltpu.VMEM((rows, 1), jnp.float32),
            pltpu.VMEM((rows, units), jnp.bfloat16),
            pltpu.VMEM((chips, rows, width), jnp.bfloat16),
            pltpu.VMEM((chips, rows, width), jnp.bfloat16),
            pltpu.VMEM((chips, rows, width), jnp.bfloat16),
            pltpu.VMEM((chips, rows, width), jnp.bfloat16),
            dma((blocks,)),
            dma((blocks,)),
            dma((blocks,)),
            dma,
            dma((chips,)),
            dma((chips,)),
            dma((blocks,)),
            dma((chips,)),
            dma((chips,)),
            dma((chips,)),
            dma((chips,)),
        ],
        compiler_params=pltpu.CompilerParams(
            collective_id=collective_id, has_side_effects=True, vmem_limit_bytes=VMEM_LIMIT
        ),
    )(own, gain.reshape(blocks, 1, width), gate, up, down)


def per_device(
    tokens,
    carried_state,
    first_gain,
    first_gate,
    first_up,
    first_down,
    mix_gain,
    query_weight,
    forget_weight,
    input_weight,
    outgate_weight,
    forget_floor,
    head_gain,
    output_weight,
    second_gain,
    second_gate,
    second_up,
    second_down,
):
    own_index = lax.axis_index(("kv", "tp"))
    group_size = lax.axis_size(("kv", "tp"))
    share_cols = tokens.shape[1]
    full_width = share_cols * group_size
    chips = lax.axis_size("kv")
    mixer_share = feed_forward(tokens, first_gain, first_gate, first_up, first_down, chips, 0)
    share_wide = mixer_share.astype(jnp.float32)
    mix_scaled = (
        share_wide * lax.dynamic_slice_in_dim(mix_gain, own_index * share_cols, share_cols)
    ).astype(jnp.bfloat16)
    state_rows, head_count, key_size, value_size = carried_state.shape
    squares = jnp.sum(share_wide * share_wide, axis=1, keepdims=True)
    coarse = squares.astype(jnp.bfloat16)
    rest = (squares - coarse.astype(jnp.float32)).astype(jnp.bfloat16)
    lanes = jnp.concatenate([coarse, rest, jnp.zeros((coarse.shape[0], 126), jnp.bfloat16)], axis=1)
    projected = lax.psum_scatter(
        jnp.concatenate(
            [
                jnp.dot(mix_scaled, weight_part, preferred_element_type=jnp.float32).astype(
                    jnp.bfloat16
                )
                for weight_part in (query_weight, forget_weight, input_weight, outgate_weight)
            ]
            + [lanes],
            axis=1,
        ),
        ("kv", "tp"),
        scatter_dimension=0,
        tiled=True,
    ).astype(jnp.float32)
    own_squares = projected[:, -128:-127] + projected[:, -127:-126]
    projected = projected[:, :-128] * lax.rsqrt(own_squares / full_width + epsilon)
    key_width = head_count * key_size
    value_width = head_count * value_size
    query_act = projected[:, :key_width].reshape(state_rows, head_count, key_size)
    forget_pre = projected[:, key_width : 2 * key_width].reshape(state_rows, head_count, key_size)
    input_val = projected[:, 2 * key_width : 2 * key_width + value_width].reshape(
        state_rows, head_count, value_size
    )
    gate_pre = projected[:, 2 * key_width + value_width :].reshape(
        state_rows, head_count, value_size
    )
    floor_grid = forget_floor.reshape(head_count, key_size)
    forget = floor_grid + (1.0 - floor_grid) * jax.nn.sigmoid(forget_pre)
    next_state = (
        forget[..., None] * carried_state + (1.0 - forget)[..., None] * input_val[:, :, None, :]
    )
    readout = jnp.sum(next_state * jax.nn.silu(query_act)[..., None], axis=2)
    normed = (
        readout
        * lax.rsqrt(jnp.mean(readout * readout, axis=-1, keepdims=True) + epsilon)
        * head_gain
    )
    mixer_out = (
        (normed * jax.nn.silu(gate_pre)).reshape(state_rows, value_width).astype(jnp.bfloat16)
    )
    update = jnp.dot(
        gather_rows(mixer_out, chips, 1).reshape(state_rows * group_size, value_width),
        output_weight,
        preferred_element_type=jnp.float32,
    )
    middle = (share_wide + update).astype(jnp.bfloat16)
    layer_out = feed_forward(middle, second_gain, second_gate, second_up, second_down, chips, 2)
    return (layer_out, next_state)


def solution(mesh):
    in_specs = (
        P("dp", ("kv", "tp")),
        P(("dp", "kv", "tp"), None, None, None),
        P(),
        P(None, ("kv", "tp")),
        P(None, ("kv", "tp")),
        P(("kv", "tp"), None),
        P(),
        P(("kv", "tp"), None),
        P(("kv", "tp"), None),
        P(("kv", "tp"), None),
        P(("kv", "tp"), None),
        P(),
        P(),
        P(None, ("kv", "tp")),
        P(),
        P(None, ("kv", "tp")),
        P(None, ("kv", "tp")),
        P(("kv", "tp"), None),
    )
    out_specs = (P("dp", ("kv", "tp")), P(("dp", "kv", "tp"), None, None, None))
    return jax.shard_map(
        per_device, mesh=mesh, in_specs=in_specs, out_specs=out_specs, check_vma=False
    )
```

```python
import functools

import jax
import jax.numpy as jnp
from jax import lax
from jax.experimental import pallas as pl
from jax.experimental.pallas import tpu as pltpu
from jax.sharding import PartitionSpec as P

epsilon = 1e-06
MESH = pl.DeviceIdType.MESH
VMEM_LIMIT = 62 * 1024 * 1024


def remote(src, dst, send_sem, recv_sem, kv, tp):
    return pltpu.make_async_remote_copy(
        src_ref=src,
        dst_ref=dst,
        send_sem=send_sem,
        recv_sem=recv_sem,
        device_id={"kv": kv, "tp": tp},
        device_id_type=MESH,
    )


def greet(me, core, chips):
    barrier = pltpu.get_barrier_semaphore()
    pl.semaphore_signal(
        barrier, inc=1, device_id={"kv": me, "tp": 1 - core}, device_id_type=MESH
    )
    for step in range(1, chips):
        pl.semaphore_signal(
            barrier,
            inc=1,
            device_id={"kv": lax.rem(me + step, chips), "tp": core},
            device_id_type=MESH,
        )
    pl.semaphore_wait(barrier, chips)


def gather_kernel(chips, own_ref, full_ref, local_sem, chip_send, sib_send, recv_sem):
    me = lax.axis_index("kv")
    core = lax.axis_index("tp")
    mine = me * 2 + core
    local = pltpu.make_async_copy(own_ref, full_ref.at[mine], local_sem)
    local.start()
    greet(me, core, chips)
    sends = []
    for step in range(1, chips):
        peer = lax.rem(me + chips - step, chips)
        copy = remote(
            own_ref, full_ref.at[mine], chip_send.at[step], recv_sem.at[mine], peer, core
        )
        copy.start()
        sends.append(copy)
    copy = remote(own_ref, full_ref.at[mine], sib_send.at[0], recv_sem.at[mine], me, 1 - core)
    copy.start()
    sends.append(copy)
    for step in range(1, chips):
        slot = lax.rem(me + step, chips) * 2 + core
        remote(
            full_ref.at[slot], full_ref.at[slot], chip_send.at[0], recv_sem.at[slot], me, 1 - core
        ).wait_recv()
        copy = remote(
            full_ref.at[slot], full_ref.at[slot], sib_send.at[step], recv_sem.at[slot], me, 1 - core
        )
        copy.start()
        sends.append(copy)
    for step in range(chips):
        slot = lax.rem(me + step, chips) * 2 + 1 - core
        remote(
            full_ref.at[slot], full_ref.at[slot], chip_send.at[0], recv_sem.at[slot], me, 1 - core
        ).wait_recv()
    for copy in sends:
        copy.wait_send()
    local.wait()


def gather_rows(own, chips, collective_id):
    blocks = chips * 2
    return pl.pallas_call(
        functools.partial(gather_kernel, chips),
        out_shape=jax.ShapeDtypeStruct((blocks,) + own.shape, own.dtype),
        in_specs=[pl.BlockSpec(memory_space=pltpu.VMEM)],
        out_specs=pl.BlockSpec(memory_space=pltpu.VMEM),
        scratch_shapes=[
            pltpu.SemaphoreType.DMA,
            pltpu.SemaphoreType.DMA((chips,)),
            pltpu.SemaphoreType.DMA((chips,)),
            pltpu.SemaphoreType.DMA((blocks,)),
        ],
        compiler_params=pltpu.CompilerParams(
            collective_id=collective_id, has_side_effects=True, vmem_limit_bytes=VMEM_LIMIT
        ),
    )(own)


def block_kernel(
    chips,
    own_ref,
    gain_ref,
    gate_hbm,
    up_hbm,
    down_hbm,
    out_ref,
    gate_w,
    up_w,
    down_w,
    cols,
    gate_acc,
    up_acc,
    squares,
    hidden,
    sib_out,
    sib_in,
    chip_out,
    chip_in,
    gate_sem,
    up_sem,
    down_sem,
    local_sem,
    chip_send,
    sib_send,
    recv_sem,
    sib_out_sem,
    sib_in_sem,
    chip_out_sem,
    chip_in_sem,
):
    me = lax.axis_index("kv")
    core = lax.axis_index("tp")
    mine = me * 2 + core
    rows, width = own_ref.shape
    full_width = width * chips * 2

    def gate_copy(j):
        at = pl.ds(pl.multiple_of(j * width, width), width)
        return pltpu.make_async_copy(gate_hbm.at[at, :], gate_w.at[j], gate_sem.at[j])

    def up_copy(j):
        at = pl.ds(pl.multiple_of(j * width, width), width)
        return pltpu.make_async_copy(up_hbm.at[at, :], up_w.at[j], up_sem.at[j])

    def down_copy(j):
        at = pl.ds(pl.multiple_of(j * width, width), width)
        return pltpu.make_async_copy(down_hbm.at[:, at], down_w.at[j], down_sem.at[j])

    local = pltpu.make_async_copy(own_ref, cols.at[mine], local_sem)
    local.start()

    @pl.loop(0, chips)
    def _(step):
        q = lax.rem(me + step, chips)
        for c in (core, 1 - core):
            gate_copy(q * 2 + c).start()
            up_copy(q * 2 + c).start()

    greet(me, core, chips)

    def share_copy(step):
        return remote(
            own_ref,
            cols.at[mine],
            chip_send.at[step],
            recv_sem.at[mine],
            lax.rem(me + chips - step, chips),
            core,
        )

    def pass_copy(slot, step):
        return remote(
            cols.at[slot], cols.at[slot], sib_send.at[step], recv_sem.at[slot], me, 1 - core
        )

    @pl.loop(1, chips)
    def _(step):
        share_copy(step).start()

    @pl.loop(0, chips)
    def _(step):
        q = lax.rem(me + 1 + step, chips)
        for c in (1 - core, core):
            down_copy(q * 2 + c).start()

    gate_acc[...] = jnp.zeros_like(gate_acc)
    up_acc[...] = jnp.zeros_like(up_acc)
    squares[...] = jnp.zeros_like(squares)
    local.wait()

    def take(j):
        block = cols[j].astype(jnp.float32)
        squares[...] += jnp.sum(block * block, axis=1, keepdims=True)
        scaled = (block * gain_ref[j]).astype(jnp.bfloat16)
        gate_copy(j).wait()
        gate_acc[...] += jnp.dot(scaled, gate_w[j], preferred_element_type=jnp.float32)
        up_copy(j).wait()
        up_acc[...] += jnp.dot(scaled, up_w[j], preferred_element_type=jnp.float32)

    @pl.loop(0, chips * 2)
    def _(turn):
        step = lax.div(turn, 2)
        other = lax.rem(turn, 2)
        q = lax.rem(me + step, chips)
        slot = q * 2 + lax.rem(core + other, 2)

        @pl.when(turn > 0)
        def _():
            pass_copy(slot, step).wait_recv()

        @pl.when(other == 0)
        def _():
            pass_copy(slot, step).start()

        take(slot)

    tile = 32

    @pl.loop(0, rows // tile)
    def _(i):
        at = pl.ds(pl.multiple_of(i * tile, tile), tile)
        row_scale = lax.rsqrt(squares[at, :] / full_width + epsilon)
        gate = row_scale * gate_acc[at, :]
        hidden[at, :] = (gate * jax.nn.sigmoid(gate) * (row_scale * up_acc[at, :])).astype(
            jnp.bfloat16
        )

    def branch(j):
        down_copy(j).wait()
        return 0.5 * jnp.dot(hidden[...], down_w[j], preferred_element_type=jnp.float32)

    def sib_copy(q):
        return remote(
            sib_out.at[q], sib_in.at[q], sib_out_sem.at[q], sib_in_sem.at[q], me, 1 - core
        )

    def chip_copy(q):
        return remote(
            chip_out.at[q], chip_in.at[me], chip_out_sem.at[q], chip_in_sem.at[me], q, core
        )

    @pl.loop(0, chips)
    def _(step):
        q = lax.rem(me + 1 + step, chips)
        sib_out[q] = branch(q * 2 + 1 - core).astype(jnp.bfloat16)
        sib_copy(q).start()
        part = branch(q * 2 + core)
        sib_copy(q).wait_recv()
        chip_out[q] = (part + sib_in[q].astype(jnp.float32)).astype(jnp.bfloat16)

        @pl.when(step < chips - 1)
        def _():
            chip_copy(q).start()

        @pl.when(step == chips - 1)
        def _():
            gate_acc[:, :width] = part + sib_in[q].astype(jnp.float32)

    total = gate_acc[:, :width] + own_ref[...].astype(jnp.float32)
    for step in range(1, chips):
        q = lax.rem(me + step, chips)
        remote(
            chip_out.at[q], chip_in.at[q], chip_out_sem.at[q], chip_in_sem.at[q], q, core
        ).wait_recv()
        total = total + chip_in[q].astype(jnp.float32)
    out_ref[...] = total.astype(out_ref.dtype)

    @pl.loop(0, chips)
    def _(step):
        slot = lax.rem(me + step, chips) * 2 + core
        pass_copy(slot, step).wait_send()
        sib_copy(step).wait_send()

    @pl.loop(1, chips)
    def _(step):
        share_copy(step).wait_send()
        chip_copy(lax.rem(me + step, chips)).wait_send()


def feed_forward(own, gain, gate, up, down, chips, collective_id):
    rows, width = own.shape
    units = gate.shape[1]
    blocks = chips * 2
    dma = pltpu.SemaphoreType.DMA
    acc_width = max(units, width)
    return pl.pallas_call(
        functools.partial(block_kernel, chips),
        out_shape=jax.ShapeDtypeStruct((rows, width), jnp.bfloat16),
        in_specs=[pl.BlockSpec(memory_space=pltpu.VMEM)] * 2
        + [pl.BlockSpec(memory_space=pl.ANY)] * 3,
        out_specs=pl.BlockSpec(memory_space=pltpu.VMEM),
        scratch_shapes=[
            pltpu.VMEM((blocks, width, units), jnp.bfloat16),
            pltpu.VMEM((blocks, width, units), jnp.bfloat16),
            pltpu.VMEM((blocks, units, width), jnp.bfloat16),
            pltpu.VMEM((blocks, rows, width), jnp.bfloat16),
            pltpu.VMEM((rows, units), jnp.float32),
            pltpu.VMEM((rows, units), jnp.float32),
            pltpu.VMEM((rows, 1), jnp.float32),
            pltpu.VMEM((rows, units), jnp.bfloat16),
            pltpu.VMEM((chips, rows, width), jnp.bfloat16),
            pltpu.VMEM((chips, rows, width), jnp.bfloat16),
            pltpu.VMEM((chips, rows, width), jnp.bfloat16),
            pltpu.VMEM((chips, rows, width), jnp.bfloat16),
            dma((blocks,)),
            dma((blocks,)),
            dma((blocks,)),
            dma,
            dma((chips,)),
            dma((chips,)),
            dma((blocks,)),
            dma((chips,)),
            dma((chips,)),
            dma((chips,)),
            dma((chips,)),
        ],
        compiler_params=pltpu.CompilerParams(
            collective_id=collective_id, has_side_effects=True, vmem_limit_bytes=VMEM_LIMIT
        ),
    )(own, gain.reshape(blocks, 1, width), gate, up, down)


def state_kernel(old_ref, forget_ref, query_ref, value_ref, new_ref, readout_ref):
    batch, heads = old_ref.shape[:2]
    for s in range(batch):
        for h in range(heads):
            value = value_ref[s, h : h + 1, :]
            new = value + forget_ref[s, :, h : h + 1] * (old_ref[s, h] - value)
            new_ref[s, h] = new
            readout_ref[s, h : h + 1, :] = jnp.sum(
                new * query_ref[s, :, h : h + 1], axis=0, keepdims=True
            )


def update_state(carried, forget, query, value):
    rows, heads, keys, values = carried.shape
    batch = 2 if rows % 2 == 0 else 1
    cells = rows * heads * keys * values
    return pl.pallas_call(
        state_kernel,
        grid=(rows // batch,),
        out_shape=(
            jax.ShapeDtypeStruct(carried.shape, jnp.float32),
            jax.ShapeDtypeStruct((rows, heads, values), jnp.float32),
        ),
        in_specs=[
            pl.BlockSpec((batch, heads, keys, values), lambda i: (i, 0, 0, 0)),
            pl.BlockSpec((batch, keys, heads), lambda i: (i, 0, 0)),
            pl.BlockSpec((batch, keys, heads), lambda i: (i, 0, 0)),
            pl.BlockSpec((batch, heads, values), lambda i: (i, 0, 0)),
        ],
        out_specs=(
            pl.BlockSpec((batch, heads, keys, values), lambda i: (i, 0, 0, 0)),
            pl.BlockSpec((batch, heads, values), lambda i: (i, 0, 0)),
        ),
        compiler_params=pltpu.CompilerParams(vmem_limit_bytes=32 * 1024 * 1024),
        cost_estimate=pl.CostEstimate(
            flops=5 * cells, bytes_accessed=8 * cells, transcendentals=0
        ),
    )(carried, forget.swapaxes(1, 2), query.swapaxes(1, 2), value)


def per_device(
    tokens,
    carried_state,
    first_gain,
    first_gate,
    first_up,
    first_down,
    mix_gain,
    query_weight,
    forget_weight,
    input_weight,
    outgate_weight,
    forget_floor,
    head_gain,
    output_weight,
    second_gain,
    second_gate,
    second_up,
    second_down,
):
    own_index = lax.axis_index(("kv", "tp"))
    group_size = lax.axis_size(("kv", "tp"))
    share_cols = tokens.shape[1]
    full_width = share_cols * group_size
    chips = lax.axis_size("kv")
    mixer_share = feed_forward(tokens, first_gain, first_gate, first_up, first_down, chips, 0)
    share_wide = mixer_share.astype(jnp.float32)
    mix_scaled = (
        share_wide * lax.dynamic_slice_in_dim(mix_gain, own_index * share_cols, share_cols)
    ).astype(jnp.bfloat16)
    state_rows, head_count, key_size, value_size = carried_state.shape
    squares = jnp.sum(share_wide * share_wide, axis=1).reshape(-1, 128)
    lines = squares.shape[0]
    padded = jnp.pad(squares, ((0, -lines % 8), (0, 0)))
    squares = jnp.sum(gather_rows(padded, chips, 3), axis=0)[:lines].reshape(-1)
    projected = lax.psum_scatter(
        jnp.concatenate(
            [
                jnp.dot(mix_scaled, weight_part, preferred_element_type=jnp.float32)
                for weight_part in (query_weight, forget_weight, input_weight, outgate_weight)
            ],
            axis=1,
        ).astype(jnp.bfloat16),
        ("kv", "tp"),
        scatter_dimension=0,
        tiled=True,
    ).astype(jnp.float32)
    own_squares = lax.dynamic_slice_in_dim(squares, own_index * state_rows, state_rows)
    projected = projected * lax.rsqrt(own_squares / full_width + epsilon)[:, None]
    key_width = head_count * key_size
    value_width = head_count * value_size
    query_act = projected[:, :key_width].reshape(state_rows, head_count, key_size)
    forget_pre = projected[:, key_width : 2 * key_width].reshape(state_rows, head_count, key_size)
    input_val = projected[:, 2 * key_width : 2 * key_width + value_width].reshape(
        state_rows, head_count, value_size
    )
    gate_pre = projected[:, 2 * key_width + value_width :].reshape(
        state_rows, head_count, value_size
    )
    floor_grid = forget_floor.reshape(head_count, key_size)
    forget = floor_grid + (1.0 - floor_grid) * jax.nn.sigmoid(forget_pre)
    next_state, readout = update_state(carried_state, forget, jax.nn.silu(query_act), input_val)
    normed = (
        readout
        * lax.rsqrt(jnp.mean(readout * readout, axis=-1, keepdims=True) + epsilon)
        * head_gain
    )
    mixer_out = (
        (normed * jax.nn.silu(gate_pre)).reshape(state_rows, value_width).astype(jnp.bfloat16)
    )
    update = jnp.dot(
        gather_rows(mixer_out, chips, 1).reshape(state_rows * group_size, value_width),
        output_weight,
        preferred_element_type=jnp.float32,
    )
    middle = (share_wide + update).astype(jnp.bfloat16)
    layer_out = feed_forward(middle, second_gain, second_gate, second_up, second_down, chips, 2)
    return (layer_out, next_state)


def solution(mesh):
    in_specs = (
        P("dp", ("kv", "tp")),
        P(("dp", "kv", "tp"), None, None, None),
        P(),
        P(None, ("kv", "tp")),
        P(None, ("kv", "tp")),
        P(("kv", "tp"), None),
        P(),
        P(("kv", "tp"), None),
        P(("kv", "tp"), None),
        P(("kv", "tp"), None),
        P(("kv", "tp"), None),
        P(),
        P(),
        P(None, ("kv", "tp")),
        P(),
        P(None, ("kv", "tp")),
        P(None, ("kv", "tp")),
        P(("kv", "tp"), None),
    )
    out_specs = (P("dp", ("kv", "tp")), P(("dp", "kv", "tp"), None, None, None))
    return jax.shard_map(
        per_device, mesh=mesh, in_specs=in_specs, out_specs=out_specs, check_vma=False
    )
```
